32 devices in a mesh: kv: 8 (over z, x), tp: 4 (over y, core).
Axes of the slice: x: 2, y: 2, z: 4, core: 2. Of those that a mesh axis runs over, the one named last changes fastest.
Arguments:
- hidden_rows: bfloat16 [28, 4096], P(None, ('kv', 'tp')), may hold values from -6 to 6
- first_gain: float32 [4096], P('kv'), may hold values from 0.1 to 1.9
- first_gate: bfloat16 [4096, 11264], P('kv', 'tp'), may hold values from -0.125 to 0.125
- first_up: bfloat16 [4096, 11264], P('kv', 'tp'), may hold values from -0.125 to 0.125
- first_down: bfloat16 [11264, 4096], P('tp', 'kv'), may hold values from -0.078125 to 0.078125
- mix_gain: float32 [4096], P('kv'), may hold values from 0.1 to 1.9
- query_weight: bfloat16 [4096, 2048], P('kv', 'tp'), may hold values from -0.09375 to 0.09375
- key_weight: bfloat16 [4096, 2048], P('kv', 'tp'), may hold values from -0.09375 to 0.09375
- value_weight: bfloat16 [4096, 2048], P('kv', 'tp'), may hold values from -0.09375 to 0.09375
- forget_weight: bfloat16 [4096, 16], P('kv'), may hold values from -0.09375 to 0.09375
- forget_bias: float32 [16], replicated, may hold values from -8 to 2
- out_weight: bfloat16 [2048, 4096], P('tp', 'kv'), may hold values from -0.5 to 0.5
- second_gain: float32 [4096], P('kv'), may hold values from 0.1 to 1.9
- second_gate: bfloat16 [4096, 11264], P('kv', 'tp'), may hold values from -0.125 to 0.125
- second_up: bfloat16 [4096, 11264], P('kv', 'tp'), may hold values from -0.125 to 0.125
- second_down: bfloat16 [11264, 4096], P('tp', 'kv'), may hold values from -0.078125 to 0.078125
- cache_keys: bfloat16 [28, 2048, 2048], P(None, 'kv', 'tp'), may hold values from -48 to 48
- cache_values: bfloat16 [28, 2048, 2048], P(None, 'kv', 'tp'), may hold values from -6 to 6
- cache_gates: float32 [28, 16, 2048], P(None, 'tp', 'kv'), may hold values from -1 to 0
- lengths: int32 [28], replicated, may hold values from 1 to 2048, 16384 in all
Outputs:
- out_rows: bfloat16 [28, 4096], P(None, ('kv', 'tp'))
The draws below stay inside these ranges and needn't reach their ends.
Inputs may be any that keep to these rules, and one draw needn't show every extreme that they name: Sequence b uses cache positions 0 to lengths[b] - 1; some sequence uses all 2048.
All inputs are finite; a program needn't handle non-finite values.
Results may differ from the reference program's by a relative error of at most 0.014.
Values may be sent and summed in bfloat16 or wider, within the bound.
No kernel may reach another device: no remote copies, remote signals or barrier semaphores. Data moves between devices by JAX's collectives and lax.ppermute only.
A program may use at most 128 MiB of HBM per device.

```python
import math
import jax
import jax.numpy as jnp
import numpy as np
from jax import lax

D = 4096
FF = 11264
HEADS = 16
HEAD_DIM = 128
SEQS = 28
POS_DEV = 256
LENGTH = 2048


def draw_cache_keys(key, part):
    base = jax.random.normal(jax.random.fold_in(key, 11), (SEQS, LENGTH, HEADS, HEAD_DIM), jnp.float32)
    base = jnp.clip(base, -48.0, 48.0)
    return base.reshape(SEQS, LENGTH, HEADS * HEAD_DIM).astype(jnp.bfloat16)


def draw_cache_gates(key, part):
    fast_share = 0.5
    fast = jax.random.uniform(jax.random.fold_in(key, 21), (HEADS,)) < fast_share
    fast_rate = jnp.exp(jax.random.uniform(jax.random.fold_in(key, 22), (HEADS,), jnp.float32, math.log(1.0 / 100.0), math.log(1.0 / 30.0)))
    slow_rate = jnp.exp(jax.random.uniform(jax.random.fold_in(key, 23), (HEADS,), jnp.float32, math.log(0.5), math.log(1.0))) / LENGTH
    rate = jnp.where(fast, fast_rate, slow_rate)
    spread = jnp.where(fast, math.log(4.0), math.log(10.0))
    coords = jax.random.uniform(jax.random.fold_in(key, 24), (SEQS, HEADS, LENGTH // POS_DEV), jnp.float32, -1.0, 1.0)
    block_factor = jnp.exp(coords * spread[None, :, None])
    block_factor = jnp.repeat(block_factor, POS_DEV, axis=2)
    noise = jax.random.uniform(jax.random.fold_in(key, 25), (SEQS, HEADS, LENGTH), jnp.float32, 0.5, 1.5)
    values = -(rate[None, :, None] * block_factor * noise)
    return jnp.clip(values, -1.0, 0.0)


def strengthened(drawn, own_key, source, target, shards_of, factor):
    owner, partner = [(jnp.arange(drawn.shape[dim]) // (drawn.shape[dim] // shards_of)).reshape([-1 if axis == dim else 1 for axis in range(drawn.ndim)]) for dim in (source, target)]
    chosen = jax.random.permutation(own_key, shards_of)[partner]
    strong = (owner == chosen) | (owner == (partner + shards_of // 2) % shards_of)
    return jnp.where(strong, factor * drawn, drawn)


def level_of(rng, extent, pieces, smallest, top_value):
    level, own = 1.0, jax.random.fold_in(rng, 6)
    for axis_at, shards_of in pieces:
        heights = jnp.exp(jax.random.uniform(jax.random.fold_in(own, axis_at), (shards_of,), jnp.float32, smallest / len(pieces), top_value / len(pieces)))
        level = level * jnp.repeat(heights, extent[axis_at] // shards_of).reshape([-1 if axis == axis_at else 1 for axis in range(len(extent))])
    return level


def split_up(number_of, total, most, lean):
    loads = [(1 << 20) // math.isqrt(standing ** lean) + 1 for standing in range(2, number_of + 1)]
    rest, counts = total - most - (number_of - 1), [1] * (number_of - 1)
    while rest > 0:
        movable = [i for i in range(number_of - 1) if counts[i] < most]
        whole, left = sum([loads[i] for i in movable]), rest
        for i in movable:
            more = min(most - counts[i], max(1, left * loads[i] // whole), rest)
            counts[i] = counts[i] + more
            rest = rest - more
    return np.array([most] + counts)


def ragged(stream_key, count, total, reach, slope):
    if count == 2:
        one = jax.random.randint(stream_key, (), max(1, total - reach), min(reach, total - 1) + 1)
        return jnp.stack([one, total - one])
    sizes = jnp.asarray(split_up(count, total, reach, slope), jnp.int32)
    couples = (count - 1) // 2
    giver, sink = sizes[1:1 + 2 * couples:2], sizes[2:2 + 2 * couples:2]
    room = jnp.minimum(giver - 1, reach - sink)
    moved = jax.random.randint(jax.random.fold_in(stream_key, 1), (couples,), 0, 1 << 20) % (room + 1)
    sizes = sizes.at[1:1 + 2 * couples:2].set(giver - moved).at[2:2 + 2 * couples:2].set(sink + moved)
    return sizes[jax.random.permutation(jax.random.fold_in(stream_key, 2), count)]


def bell_draw(rng, dims, scale, most, shards=(), held_as=jnp.bfloat16):
    values = scale * jax.random.normal(rng, dims, jnp.float32)
    if shards:
        values = values * level_of(rng, dims, shards, -0.22, 0.18)
    return jnp.clip(values, -most, most).astype(held_as)


def gaussian_with(rng, dims, deviation, most, pieces, heavy, kind=jnp.bfloat16):
    array = deviation * jax.random.normal(rng, dims, jnp.float32)
    if pieces:
        array = array * level_of(rng, dims, pieces, -0.22, 0.18)
    return jnp.clip(strengthened(array, jax.random.fold_in(rng, 3), *heavy), -most, most).astype(kind)


def setup_inputs(seed: int = 0) -> dict:
    splits = jax.random.split(jax.random.key(seed), 21)
    hidden_rows = bell_draw(splits[0], (SEQS, D), 1.0, 6.0, ((1, 32),))
    first_gain = jnp.clip(1.0 + 0.18 * jax.random.normal(splits[1], (D,), jnp.float32), 0.1, 1.9)
    first_gate = gaussian_with(splits[2], (D, FF), D ** -0.5, 0.125, ((0, 8), (1, 4)), (0, 1, 8, 2.0))
    first_up = gaussian_with(splits[3], (D, FF), D ** -0.5, 0.125, ((0, 8), (1, 4)), (0, 1, 8, 2.0))
    first_down = gaussian_with(splits[4], (FF, D), FF ** -0.5, 0.078125, ((0, 4), (1, 8)), (0, 1, 8, 2.0))
    mix_gain = jnp.clip(1.0 + 0.18 * jax.random.normal(splits[5], (D,), jnp.float32), 0.1, 1.9)
    query_weight = bell_draw(splits[6], (D, HEADS * HEAD_DIM), D ** -0.5, 0.09375, ((0, 8), (1, 4)))
    key_weight = bell_draw(splits[7], (D, HEADS * HEAD_DIM), D ** -0.5, 0.09375, ((0, 8), (1, 4)))
    value_weight = bell_draw(splits[8], (D, HEADS * HEAD_DIM), D ** -0.5, 0.09375, ((0, 8), (1, 4)))
    forget_weight = bell_draw(splits[9], (D, HEADS), D ** -0.5, 0.09375, ((0, 8),))
    forget_bias = jnp.clip(jax.random.uniform(splits[10], (HEADS,), jnp.float32, -8.0, 2.0), -8.0, 2.0)
    out_weight = bell_draw(splits[11], (HEADS * HEAD_DIM, D), HEAD_DIM ** -0.5, 0.5, ((0, 4), (1, 8)))
    second_gain = jnp.clip(1.0 + 0.18 * jax.random.normal(splits[12], (D,), jnp.float32), 0.1, 1.9)
    second_gate = gaussian_with(splits[13], (D, FF), D ** -0.5, 0.125, ((0, 8), (1, 4)), (0, 1, 8, 2.0))
    second_up = gaussian_with(splits[14], (D, FF), D ** -0.5, 0.125, ((0, 8), (1, 4)), (0, 1, 8, 2.0))
    second_down = gaussian_with(splits[15], (FF, D), FF ** -0.5, 0.078125, ((0, 4), (1, 8)), (0, 1, 8, 2.0))
    cache_keys = draw_cache_keys(jax.random.fold_in(splits[20], 71), 0)
    cache_values = bell_draw(splits[17], (SEQS, LENGTH, HEADS * HEAD_DIM), 1.0, 6.0, ((1, 8), (2, 4)))
    cache_gates = draw_cache_gates(jax.random.fold_in(splits[20], 71), 0)
    lengths = ragged(splits[19], SEQS, SEQS * LENGTH // 4 + LENGTH, LENGTH, 2).astype(jnp.int32)
    return dict(hidden_rows=hidden_rows, first_gain=first_gain, first_gate=first_gate, first_up=first_up, first_down=first_down, mix_gain=mix_gain, query_weight=query_weight, key_weight=key_weight, value_weight=value_weight, forget_weight=forget_weight, forget_bias=forget_bias, out_weight=out_weight, second_gain=second_gain, second_gate=second_gate, second_up=second_up, second_down=second_down, cache_keys=cache_keys, cache_values=cache_values, cache_gates=cache_gates, lengths=lengths)


EPS = 1e-06
FLOOR = -1e+30

def half_block(rows, gain, w_gate, w_up, w_down):
    rows32 = rows.astype(jnp.float32)
    scaled = (rows32 * gain).astype(jnp.bfloat16)
    rscale = lax.rsqrt(lax.optimization_barrier(jnp.mean(rows32 * rows32, axis=1, keepdims=True)) + EPS)
    gate = jnp.dot(scaled, w_gate, preferred_element_type=jnp.float32) * rscale
    up_act = jnp.dot(scaled, w_up, preferred_element_type=jnp.float32) * rscale
    hidden = (jax.nn.silu(gate) * up_act).astype(jnp.bfloat16)
    down_sum = jnp.dot(hidden, w_down, preferred_element_type=jnp.float32)
    return (rows32 + 0.5 * down_sum).astype(jnp.bfloat16)

def mixing(rows, gain, query_weight, key_weight, value_weight, forget_weight, forget_bias, out_weight, cache_keys, cache_values, cache_gates, lengths):
    rows32 = rows.astype(jnp.float32)
    scaled = (rows32 * gain).astype(jnp.bfloat16)
    rscale = lax.rsqrt(lax.optimization_barrier(jnp.mean(rows32 * rows32, axis=1, keepdims=True)) + EPS)
    seqs = rows.shape[0]
    heads = forget_bias.shape[0]
    width = query_weight.shape[1]
    head_dim = width // heads
    query = lax.optimization_barrier((jnp.dot(scaled, query_weight, preferred_element_type=jnp.float32) * rscale).astype(jnp.bfloat16))
    fresh_key = lax.optimization_barrier((jnp.dot(scaled, key_weight, preferred_element_type=jnp.float32) * rscale).astype(jnp.bfloat16))
    fresh_value = lax.optimization_barrier((jnp.dot(scaled, value_weight, preferred_element_type=jnp.float32) * rscale).astype(jnp.bfloat16))
    fresh_gate = jax.nn.log_sigmoid(jnp.dot(scaled, forget_weight, preferred_element_type=jnp.float32) * rscale + forget_bias)
    query32 = query.astype(jnp.float32).reshape(seqs, heads, head_dim)
    key32 = fresh_key.astype(jnp.float32).reshape(seqs, heads, head_dim)
    value32 = fresh_value.astype(jnp.float32).reshape(seqs, heads, head_dim)
    total_len = cache_gates.shape[2]
    places = jnp.arange(total_len, dtype=jnp.int32)
    live = places[None, None, :] < lengths.astype(jnp.int32)[:, None, None]
    kept = jnp.where(live, cache_gates, 0.0)
    running = jnp.cumsum(kept, axis=2)
    bias = fresh_gate[:, :, None] + (running[:, :, -1:] - running)
    factor = head_dim ** (-0.5)
    span = POS_DEV
    blocks = total_len // span

    def step(carry, index):
        top_all, mass_all, summed_all = carry
        start = (index * span).astype(jnp.int32)
        keys = lax.dynamic_slice_in_dim(cache_keys, start, span, 1).astype(jnp.float32).reshape(seqs, span, heads, head_dim)
        values = lax.dynamic_slice_in_dim(cache_values, start, span, 1).astype(jnp.float32).reshape(seqs, span, heads, head_dim)
        bias_part = lax.dynamic_slice_in_dim(bias, start, span, 2)
        live_part = lax.dynamic_slice_in_dim(live, start, span, 2)
        scores = jnp.einsum('bphd,bhd->bhp', keys, query32) * factor + bias_part
        top = lax.optimization_barrier(jnp.max(jnp.where(live_part, scores, FLOOR), axis=2))
        weights = jnp.where(live_part, jnp.exp(scores - top[:, :, None]), 0.0)
        mass = lax.optimization_barrier(jnp.sum(weights, axis=2))
        rounded = lax.optimization_barrier(weights.astype(jnp.bfloat16)).astype(jnp.float32)
        summed = jnp.einsum('bhp,bphd->bhd', rounded, values)
        peak = jnp.maximum(top_all, top)
        old_part = jnp.exp(top_all - peak)
        new_part = jnp.exp(top - peak)
        return ((peak, mass_all * old_part + mass * new_part, summed_all * old_part[:, :, None] + summed * new_part[:, :, None]), None)
    start_carry = (jnp.full((seqs, heads), FLOOR, jnp.float32), jnp.zeros((seqs, heads), jnp.float32), jnp.zeros((seqs, heads, head_dim), jnp.float32))
    (top, mass, summed), _ = lax.scan(step, start_carry, jnp.arange(blocks, dtype=jnp.int32))
    own = lax.optimization_barrier(jnp.sum(query32 * key32, axis=2)) * factor
    peak = jnp.maximum(top, own)
    keep = jnp.exp(top - peak)
    fresh = jnp.exp(own - peak)
    attended = ((summed * keep[:, :, None] + value32 * fresh[:, :, None]) / (mass * keep + fresh)[:, :, None]).astype(jnp.bfloat16).reshape(seqs, width)
    mixed = jnp.dot(attended, out_weight, preferred_element_type=jnp.float32)
    return (rows32 + mixed).astype(jnp.bfloat16)

def reference(hidden_rows, first_gain, first_gate, first_up, first_down, mix_gain, query_weight, key_weight, value_weight, forget_weight, forget_bias, out_weight, second_gain, second_gate, second_up, second_down, cache_keys, cache_values, cache_gates, lengths):
    mid_rows = half_block(hidden_rows, first_gain, first_gate, first_up, first_down)
    after_rows = mixing(mid_rows, mix_gain, query_weight, key_weight, value_weight, forget_weight, forget_bias, out_weight, cache_keys, cache_values, cache_gates, lengths)
    return half_block(after_rows, second_gain, second_gate, second_up, second_down)
```

```python
import functools

import jax
import jax.numpy as jnp
from jax import lax
from jax.experimental import pallas as pl
from jax.experimental.pallas import tpu as pltpu
from jax.sharding import PartitionSpec as P

D = 4096
HEAD_DIM = 128
LANES = 128

EPS = 1e-06
FLOOR = -1e30
DEAD = -1e29


def pieces(x, count):
    out = []
    rest = x
    for _ in range(count):
        part = lax.reduce_precision(rest, 8, 7)
        out.append(part.astype(jnp.bfloat16))
        rest = rest - part
    return out


def exchange(x, axis):
    return lax.all_to_all(x, axis, 0, 0)


def spread(x, axis):
    everyone = jnp.broadcast_to(x[None], (lax.axis_size(axis),) + x.shape)
    return exchange(everyone, axis)


def row_share(rows):
    devices = lax.axis_size("kv")
    return devices, -(-rows // devices)


def padded_to(x, rows):
    return jnp.pad(x, ((0, rows - x.shape[0]), (0, 0)))


def widen(shard):
    return lax.all_gather(shard, "tp", axis=1, tiled=True)


def scaled_rows(block, gain):
    block32 = block.astype(jnp.float32)
    scaled = (block32 * gain).astype(jnp.bfloat16)
    squares = jnp.sum(block32 * block32, axis=1, keepdims=True)
    return (scaled, squares)


def feed_forward(block, gain, w_gate, w_up, w_down):
    seqs = block.shape[0]
    units = w_gate.shape[1]
    devices, share = row_share(seqs)
    scaled, squares = scaled_rows(block, gain)
    gate = jnp.dot(scaled, w_gate, preferred_element_type=jnp.float32)
    up_act = jnp.dot(scaled, w_up, preferred_element_type=jnp.float32)
    squares = jnp.concatenate(pieces(squares, 2), axis=1)
    squares = jnp.pad(squares, ((0, 0), (0, LANES - squares.shape[1])))
    sent = jnp.concatenate(
        [gate.astype(jnp.bfloat16), up_act.astype(jnp.bfloat16), squares], axis=1
    )
    sent = padded_to(sent, devices * share).reshape(devices, share, sent.shape[1])
    total = jnp.sum(exchange(sent, "kv").astype(jnp.float32), axis=0)
    squares = jnp.sum(total[:, 2 * units :], axis=1, keepdims=True)
    rscale = lax.rsqrt(squares / D + EPS)
    hidden = jax.nn.silu(total[:, :units] * rscale) * (total[:, units : 2 * units] * rscale)
    hidden = spread(hidden.astype(jnp.bfloat16), "kv")
    hidden = hidden.reshape(devices * share, units)[:seqs]
    return jnp.dot(hidden, w_down, preferred_element_type=jnp.float32)


def project_kernel(x_ref, wq_ref, wk_ref, wv_ref, out_ref):
    x = x_ref[...]
    width = wq_ref.shape[1]
    for at, w_ref in enumerate((wq_ref, wk_ref, wv_ref)):
        part = jnp.dot(x, w_ref[...], preferred_element_type=jnp.float32)
        out_ref[:, at * width : (at + 1) * width] = part.astype(jnp.bfloat16)


def project(scaled, wq, wk, wv):
    return pl.pallas_call(
        project_kernel,
        out_shape=jax.ShapeDtypeStruct((scaled.shape[0], 3 * wq.shape[1]), jnp.bfloat16),
    )(scaled, wq, wk, wv)


def cache_kernel(factor, q_ref, bias_ref, k_ref, v_ref, out_ref):
    group, span, width = k_ref.shape
    tall = bias_ref.shape[1]
    row = lax.broadcasted_iota(jnp.int32, (tall, width), 0)
    lane = lax.broadcasted_iota(jnp.int32, (tall, width), 1)
    own_head = (lane >= row * HEAD_DIM) & (lane < (row + 1) * HEAD_DIM)
    small_row = lax.broadcasted_iota(jnp.int32, (tall, LANES), 0)
    small_lane = lax.broadcasted_iota(jnp.int32, (tall, LANES), 1)
    for s in range(group):
        query = jnp.broadcast_to(q_ref[s], (tall, width))
        query = jnp.where(own_head, query, 0.0).astype(jnp.bfloat16)
        scores = lax.dot_general(
            query, k_ref[s], (((1,), (1,)), ((), ())), preferred_element_type=jnp.float32
        )
        bias = bias_ref[s]
        scores = scores * factor + bias
        top = jnp.max(scores, axis=1, keepdims=True)
        weights = jnp.where(bias > DEAD, jnp.exp(scores - top), 0.0)
        mass = jnp.sum(weights, axis=1, keepdims=True)
        summed = jnp.dot(
            weights.astype(jnp.bfloat16), v_ref[s], preferred_element_type=jnp.float32
        )
        summed = jnp.sum(jnp.where(own_head, summed, 0.0), axis=0, keepdims=True)
        small = jnp.where(small_lane == small_row, top, 0.0) + jnp.where(
            small_lane == small_row + tall, mass, 0.0
        )
        out_ref[s, :, :width] = summed
        out_ref[s, :, width:] = jnp.sum(small, axis=0, keepdims=True)


def cache_parts(query, bias, keys, values):
    seqs, span, width = keys.shape
    tall = bias.shape[1]
    group = max(g for g in (4, 2, 1) if seqs % g == 0)
    return pl.pallas_call(
        functools.partial(cache_kernel, HEAD_DIM ** (-0.5)),
        grid=(seqs // group,),
        in_specs=[
            pl.BlockSpec((group, 1, width), lambda i: (i, 0, 0)),
            pl.BlockSpec((group, tall, span), lambda i: (i, 0, 0)),
            pl.BlockSpec((group, span, width), lambda i: (i, 0, 0)),
            pl.BlockSpec((group, span, width), lambda i: (i, 0, 0)),
        ],
        out_specs=pl.BlockSpec((group, 1, width + LANES), lambda i: (i, 0, 0)),
        out_shape=jax.ShapeDtypeStruct((seqs, 1, width + LANES), jnp.float32),
        compiler_params=pltpu.CompilerParams(dimension_semantics=("arbitrary",)),
    )(query[:, None], bias, keys, values)


def attention(
    block,
    gain,
    query_weight,
    key_weight,
    value_weight,
    forget_weight,
    forget_bias,
    out_weight,
    cache_keys,
    cache_values,
    cache_gates,
    lengths,
):
    seqs = block.shape[0]
    width = query_weight.shape[1]
    heads = width // HEAD_DIM
    tall = -(-heads // 8) * 8
    span = cache_keys.shape[1]
    devices, share = row_share(seqs)
    rows = devices * share
    mine = lax.axis_index("kv")
    first_head = lax.axis_index("tp") * heads

    places = mine * span + jnp.arange(span, dtype=jnp.int32)
    live = places[None, None, :] < lengths[:, None, None]
    kept = jnp.where(live, cache_gates, 0.0)
    local_total = jnp.sum(kept, axis=2)
    order = jnp.arange(span, dtype=jnp.int32)
    later = (order[:, None] > order[None, :]).astype(jnp.float32)
    after = lax.dot_general(
        kept, later, (((2,), (0,)), ((), ())), precision=lax.Precision.HIGHEST
    )
    bias = jnp.where(live, after, FLOOR)
    bias = jnp.pad(bias, ((0, 0), (0, tall - heads), (0, 0)), constant_values=FLOOR)

    scaled, squares = scaled_rows(block, gain)
    own_forget = lax.dynamic_slice_in_dim(forget_weight, first_head, heads, 1)
    part_logit = jnp.dot(scaled, own_forget, preferred_element_type=jnp.float32)
    parts = project(padded_to(scaled, -(-rows // 16) * 16), query_weight, key_weight, value_weight)
    squares = jnp.concatenate(pieces(squares, 2), axis=1)
    squares = jnp.pad(squares, ((0, 0), (0, LANES - squares.shape[1])))
    for_all = jnp.concatenate([parts[:seqs, :width], squares], axis=1)
    small = jnp.concatenate(pieces(part_logit, 2) + pieces(local_total, 3), axis=1)
    small = jnp.pad(small, ((0, rows - seqs), (0, 2 * LANES - small.shape[1])))
    for_owner = jnp.concatenate([parts[:rows, width:], small], axis=1)
    sent = jnp.concatenate(
        [
            jnp.broadcast_to(for_all[None], (devices,) + for_all.shape),
            for_owner.reshape(devices, 2 * share, width + LANES),
        ],
        axis=1,
    )
    came = exchange(sent, "kv")

    total = jnp.sum(came[:, :seqs].astype(jnp.float32), axis=0)
    rscale = lax.rsqrt(jnp.sum(total[:, width:], axis=1, keepdims=True) / D + EPS)
    query = (total[:, :width] * rscale).astype(jnp.bfloat16).astype(jnp.float32)
    sent = cache_parts(query, bias, cache_keys, cache_values)
    sent = padded_to(sent[:, 0], rows)
    came_parts = exchange(sent.reshape(devices, share, width + LANES), "kv")

    own = came[:, seqs:].reshape(devices, share, 2 * (width + LANES)).astype(jnp.float32)
    totals = own[:, :, 2 * width + 2 * heads : 2 * width + 5 * heads]
    totals = jnp.sum(totals.reshape(devices, share, 3, heads), axis=2)
    place = jnp.arange(devices, dtype=jnp.int32)
    beyond = (place[:, None] < place[None, :])[:, :, None, None]
    beyond = jnp.sum(jnp.where(beyond, totals[None], 0.0), axis=1)
    own = jnp.sum(own, axis=0)
    first = mine * share
    own_rscale = lax.dynamic_slice_in_dim(padded_to(rscale, rows), first, share, 0)
    own_query = lax.dynamic_slice_in_dim(padded_to(query, rows), first, share, 0)
    fresh = (own[:, : 2 * width] * own_rscale).astype(jnp.bfloat16).astype(jnp.float32)
    fresh_key = fresh[:, :width].reshape(share, heads, HEAD_DIM)
    fresh_value = fresh[:, width:].reshape(share, heads, HEAD_DIM)
    logit = own[:, 2 * width : 2 * width + heads] + own[:, 2 * width + heads : 2 * width + 2 * heads]
    own_bias = lax.dynamic_slice_in_dim(forget_bias, first_head, heads, 0)
    fresh_gate = jax.nn.log_sigmoid(logit * own_rscale + own_bias)

    own_score = jnp.sum(own_query.reshape(share, heads, HEAD_DIM) * fresh_key, axis=2)
    own_score = own_score * HEAD_DIM ** (-0.5)
    top = came_parts[:, :, width : width + heads] + (beyond + fresh_gate[None])
    mass = came_parts[:, :, width + tall : width + tall + heads]
    summed = came_parts[:, :, :width].reshape(devices, share, heads, HEAD_DIM)
    peak = jnp.maximum(jnp.max(top, axis=0), own_score)
    keep = jnp.exp(top - peak[None])
    fresh = jnp.exp(own_score - peak)
    over = jnp.sum(summed * keep[:, :, :, None], axis=0) + fresh_value * fresh[:, :, None]
    under = jnp.sum(mass * keep, axis=0) + fresh
    attended = (over / under[:, :, None]).astype(jnp.bfloat16).reshape(share, width)
    attended = spread(attended, "kv").reshape(rows, width)[:seqs]
    return jnp.dot(attended, out_weight, preferred_element_type=jnp.float32)


def advance(block, partial_value, weight):
    total = lax.all_gather(partial_value.astype(jnp.bfloat16), "tp").astype(jnp.float32)
    total = jnp.sum(total, axis=0)
    return (block.astype(jnp.float32) + weight * total).astype(jnp.bfloat16)


def finish(block, partial_value, weight, columns):
    devices = lax.axis_size("tp")
    seqs = block.shape[0]
    sent = partial_value.astype(jnp.bfloat16).reshape(seqs, devices, columns).transpose(1, 0, 2)
    total = jnp.sum(exchange(sent, "tp").astype(jnp.float32), axis=0)
    kept = lax.dynamic_slice_in_dim(block, lax.axis_index("tp") * columns, columns, 1)
    return (kept.astype(jnp.float32) + weight * total).astype(jnp.bfloat16)


def local(
    hidden_rows,
    first_gain,
    first_gate,
    first_up,
    first_down,
    mix_gain,
    query_weight,
    key_weight,
    value_weight,
    forget_weight,
    forget_bias,
    out_weight,
    second_gain,
    second_gate,
    second_up,
    second_down,
    cache_keys,
    cache_values,
    cache_gates,
    lengths,
):
    block = widen(hidden_rows)
    partial_value = feed_forward(block, first_gain, first_gate, first_up, first_down)
    block = advance(block, partial_value, 0.5)
    partial_value = attention(
        block,
        mix_gain,
        query_weight,
        key_weight,
        value_weight,
        forget_weight,
        forget_bias,
        out_weight,
        cache_keys,
        cache_values,
        cache_gates,
        lengths,
    )
    block = advance(block, partial_value, 1.0)
    partial_value = feed_forward(block, second_gain, second_gate, second_up, second_down)
    return finish(block, partial_value, 0.5, hidden_rows.shape[1])


def solution(mesh):
    return jax.shard_map(
        local,
        mesh=mesh,
        in_specs=(
            P(None, ("kv", "tp")),
            P("kv"),
            P("kv", "tp"),
            P("kv", "tp"),
            P("tp", "kv"),
            P("kv"),
            P("kv", "tp"),
            P("kv", "tp"),
            P("kv", "tp"),
            P("kv", None),
            P(),
            P("tp", "kv"),
            P("kv"),
            P("kv", "tp"),
            P("kv", "tp"),
            P("tp", "kv"),
            P(None, "kv", "tp"),
            P(None, "kv", "tp"),
            P(None, "tp", "kv"),
            P(),
        ),
        out_specs=P(None, ("kv", "tp")),
        check_vma=False,
    )
```
